32 devices in a mesh: rep: 4 (over z), fs: 4 (over y, x), tp: 2 (over core).
Axes of the slice: x: 2, y: 2, z: 4, core: 2. Of those that a mesh axis runs over, the one named last changes fastest.
Arguments:
- tokens_in: bfloat16 [8192, 2048], P(('rep', 'fs', 'tp')), may hold values from -6 to 6
- norm_gain: float32 [2048], replicated, may hold values from 0.1 to 1.9
- gate_weight: bfloat16 [2048, 3072], P(None, ('fs', 'tp')), may hold values from -0.125 to 0.125
- up_weight: bfloat16 [2048, 3072], P(None, ('fs', 'tp')), may hold values from -0.125 to 0.125
- down_weight: bfloat16 [3072, 2048], P(('fs', 'tp')), may hold values from -0.109375 to 0.109375
- out_grad: bfloat16 [8192, 2048], P(('rep', 'fs', 'tp')), may hold values from -6 to 6
Outputs:
- grad_in: bfloat16 [8192, 2048], P(('rep', 'fs', 'tp'))
- grad_gain: float32 [2048], replicated
- grad_gate: float32 [2048, 3072], P(None, ('fs', 'tp'))
- grad_up: float32 [2048, 3072], P(None, ('fs', 'tp'))
- grad_down: float32 [3072, 2048], P(('fs', 'tp'))
The draws below stay inside these ranges and needn't reach their ends.
All inputs are finite; a program needn't handle non-finite values.
Results may differ from the reference program's by a relative error of at most 0.014.
Values may be sent and summed in bfloat16 or wider, within the bound.
A program may use at most 192 MiB of HBM per device.

```python
import jax
import jax.numpy as jnp
from jax import lax

D = 2048
FF = 3072
TOKENS = 8192
BLOCKS = 8


def strengthened(entries, key, source, target, shards_of, factor):
    def block_of(axis_at):
        return (jnp.arange(entries.shape[axis_at]) // (entries.shape[axis_at] // shards_of)).reshape((-1,) + (1,) * (entries.ndim - 1 - axis_at))

    first = jax.random.permutation(key, shards_of)[block_of(target)]
    far = (block_of(target) + shards_of // 2) % shards_of
    return jnp.where((block_of(source) == first) | (block_of(source) == far), factor * entries, entries)


def shard_levels(rng, dims, split, smallest, high):
    factor_of, own = 1.0, jax.random.fold_in(rng, 6)
    for axis_at, shards_of in split:
        draws = jnp.exp(jax.random.uniform(jax.random.fold_in(own, axis_at), (shards_of,), jnp.float32, smallest / len(split), high / len(split)))
        factor_of = factor_of * jnp.repeat(draws, dims[axis_at] // shards_of).reshape([-1 if axis == axis_at else 1 for axis in range(len(dims))])
    return factor_of


def normal_values(rng, extent, scale, most, cuts=(), held_as=jnp.bfloat16):
    drawn = jax.random.normal(rng, extent, jnp.float32) * scale
    if len(cuts) > 0:
        drawn = shard_levels(rng, extent, cuts, -0.22, 0.18) * drawn
    return jnp.clip(drawn, min=-most, max=most).astype(held_as)


def noise_with(key, dims, scale, reach, shards, heavy, dtype=jnp.bfloat16):
    array = scale * jax.random.normal(key, dims, jnp.float32)
    if shards:
        array = array * shard_levels(key, dims, shards, -0.22, 0.18)
    return jnp.clip(strengthened(array, jax.random.fold_in(key, 3), *heavy), -reach, reach).astype(dtype)


def setup_inputs(seed: int = 0) -> dict:
    key_of = jax.random.split(jax.random.key(seed), 7)
    return {
        "tokens_in": normal_values(key_of[0], (TOKENS, D), 1.0, 6.0, ((0, 32),)),
        "norm_gain": jnp.clip(1.0 + 0.18 * jax.random.normal(key_of[1], (D,), jnp.float32), 0.1, 1.9),
        "gate_weight": normal_values(key_of[2], (D, FF), D ** -0.5, 0.125, ((1, 8),)),
        "up_weight": normal_values(key_of[3], (D, FF), D ** -0.5, 0.125, ((1, 8),)),
        "down_weight": normal_values(key_of[4], (FF, D), FF ** -0.5, 0.109375, ((0, 8),)),
        "out_grad": noise_with(key_of[5], (TOKENS, D), 1.0, 6.0, ((0, 32),), (0, 1, 32, 2.75)),
    }


norm_eps = 1e-06

def reference(tokens_in, norm_gain, gate_weight, up_weight, down_weight, out_grad):
    floats = tokens_in.astype(jnp.float32)
    inverse = lax.rsqrt(lax.optimization_barrier(jnp.mean(floats * floats, axis=-1, keepdims=True)) + norm_eps)
    unit_rows = floats * inverse
    normed = (unit_rows * norm_gain).astype(jnp.bfloat16)
    gate_pre = jnp.dot(normed, gate_weight, preferred_element_type=jnp.float32)
    up_pre = jnp.dot(normed, up_weight, preferred_element_type=jnp.float32)
    sigma = jax.nn.sigmoid(gate_pre)
    active = gate_pre * sigma
    hidden = (active * up_pre).astype(jnp.bfloat16)
    grad_hidden = 0.5 * jnp.dot(out_grad, down_weight.T, preferred_element_type=jnp.float32)
    grad_gate_pre = (grad_hidden * up_pre * sigma * (1.0 + gate_pre * (1.0 - sigma))).astype(jnp.bfloat16)
    grad_up_pre = (grad_hidden * active).astype(jnp.bfloat16)
    factor = float(TOKENS) ** (-0.5)
    grad_down = jnp.dot(hidden.T, out_grad, preferred_element_type=jnp.float32) * (0.5 * factor)
    grad_gate = jnp.dot(normed.T, grad_gate_pre, preferred_element_type=jnp.float32) * factor
    grad_up = jnp.dot(normed.T, grad_up_pre, preferred_element_type=jnp.float32) * factor
    width = FF // BLOCKS
    grad_normed = jnp.zeros(floats.shape, jnp.float32)
    for block in range(BLOCKS):
        lower = block * width
        term = jnp.dot(grad_gate_pre[:, lower:lower + width], gate_weight[:, lower:lower + width].T, preferred_element_type=jnp.float32)
        term = term + jnp.dot(grad_up_pre[:, lower:lower + width], up_weight[:, lower:lower + width].T, preferred_element_type=jnp.float32)
        grad_normed = grad_normed + term.astype(jnp.bfloat16).astype(jnp.float32)
    grad_gain = lax.optimization_barrier(jnp.sum(grad_normed * unit_rows, axis=0))
    scaled = grad_normed * norm_gain
    grad_in = out_grad.astype(jnp.float32) + inverse * scaled - unit_rows * inverse * lax.optimization_barrier(jnp.mean(scaled * unit_rows, axis=-1, keepdims=True))
    return (grad_in.astype(jnp.bfloat16), grad_gain, grad_gate, grad_up, grad_down)
```

```python
import jax
import jax.numpy as jnp
from jax import lax
from jax.experimental import pallas as pl
from jax.experimental.pallas import tpu as pltpu
from jax.sharding import PartitionSpec as P

norm_eps = 1e-06
MESH = pl.DeviceIdType.MESH
F32, BF16 = jnp.float32, jnp.bfloat16
CHUNKS = 8
NT = (((1,), (1,)), ((), ()))


def flip(f, j):
    return (f % 2 + j % 2) % 2 + 2 * ((f // 2 + j // 2) % 2)


def remote(src, dst, send, recv, dev):
    return pltpu.make_async_remote_copy(
        src_ref=src, dst_ref=dst, send_sem=send, recv_sem=recv, device_id=dev, device_id_type=MESH
    )


def gather_kernel(
    x_ref, g_ref, gain_ref, gw_ref, uw_ref, dw_ref,
    normed_out, grad_out, hid_out, ggp_out, gup_out,
    xall, gall, normed, hid, ggp, gup, ssem, rsem, osem,
):
    f, t = lax.axis_index("fs"), lax.axis_index("tp")
    other = 1 - t
    rows = x_ref.shape[0]
    half = rows // 2
    to_a, to_b, to_p = {"fs": flip(f, 1)}, {"fs": flip(f, 2)}, {"tp": other}
    barrier = pltpu.get_barrier_semaphore()
    for dev in (to_a, to_b, to_p):
        pl.semaphore_signal(barrier, inc=1, device_id=dev, device_id_type=MESH)
    pl.semaphore_wait(barrier, 3)

    def pos(j, core):
        return flip(f, j) * 2 + core

    bufs = ((x_ref, xall), (g_ref, gall))
    low, high = pl.ds(0, half), pl.ds(half, half)

    def copy(n, kind, incoming=False):
        own, held = bufs[n]
        sems = (ssem.at[n, kind], rsem.at[n, kind])
        mine = pos(0, t)
        if kind == 0:
            return remote(own, held.at[pos(1, t) if incoming else mine], *sems, to_a)
        if kind == 1:
            return remote(own, held.at[pos(2, t) if incoming else mine], *sems, to_b)
        if kind == 2:
            return remote(own, held.at[pos(0, other) if incoming else mine], *sems, to_p)
        if kind == 3:
            slot = held.at[pos(3, t) if incoming else pos(1, t), high]
            return remote(slot, slot, *sems, to_b)
        if kind == 4:
            slot = held.at[pos(3, t) if incoming else pos(2, t), low]
            return remote(slot, slot, *sems, to_a)
        j = {5: 1, 6: 2, 7: 3, 8: 3}[kind]
        slot = held.at[pos(j, other if incoming else t)]
        if kind == 7:
            slot = slot.at[low]
        if kind == 8:
            slot = slot.at[high]
        return remote(slot, slot, *sems, to_p)

    for n in range(2):
        for kind in (0, 1, 2):
            copy(n, kind).start()
    xall[pos(0, t)] = x_ref[...]
    gall[pos(0, t)] = g_ref[...]

    def outs(p):
        return [
            pltpu.make_async_copy(src.at[p], dst.at[p], osem.at[i])
            for i, (src, dst) in enumerate(
                ((normed, normed_out), (gall, grad_out), (hid, hid_out), (ggp, ggp_out), (gup, gup_out))
            )
        ]

    def body(i, carry):
        @pl.when(i == 1)
        def _():
            for n in range(2):
                copy(n, 2, True).wait_recv()

        @pl.when(i == 2)
        def _():
            for n in range(2):
                copy(n, 0, True).wait_recv()
                copy(n, 3).start()
                copy(n, 5).start()
                copy(n, 1, True).wait_recv()
                copy(n, 4).start()
                copy(n, 6).start()

        @pl.when(i == 3)
        def _():
            for n in range(2):
                copy(n, 5, True).wait_recv()

        @pl.when(i == 5)
        def _():
            for n in range(2):
                copy(n, 6, True).wait_recv()

        @pl.when(i == 6)
        def _():
            for n in range(2):
                copy(n, 4, True).wait_recv()
                copy(n, 7).start()
                copy(n, 3, True).wait_recv()
                copy(n, 8).start()

        @pl.when(i == 7)
        def _():
            for n in range(2):
                copy(n, 7, True).wait_recv()
                copy(n, 8, True).wait_recv()

        p = flip(f, i // 2) * 2 + (t + i) % 2
        floats = xall[p].astype(F32)
        inverse = lax.rsqrt(jnp.mean(floats * floats, axis=-1, keepdims=True) + norm_eps)
        normed[p] = (floats * inverse * gain_ref[...]).astype(BF16)
        gate_pre = jnp.dot(normed[p], gw_ref[...], preferred_element_type=F32)
        up_pre = jnp.dot(normed[p], uw_ref[...], preferred_element_type=F32)
        grad_hidden = 0.5 * lax.dot_general(gall[p], dw_ref[...], NT, preferred_element_type=F32)
        sigma = jax.nn.sigmoid(gate_pre)
        active = gate_pre * sigma
        hid[p] = (active * up_pre).astype(BF16)
        ggp[p] = (grad_hidden * up_pre * sigma * (1.0 + gate_pre * (1.0 - sigma))).astype(BF16)
        gup[p] = (grad_hidden * active).astype(BF16)
        return carry

    lax.fori_loop(0, 8, body, 0)
    whole = [
        pltpu.make_async_copy(src, dst, osem.at[i])
        for i, (src, dst) in enumerate(
            ((normed, normed_out), (gall, grad_out), (hid, hid_out), (ggp, ggp_out), (gup, gup_out))
        )
    ]
    for c in whole:
        c.start()
    for n in range(2):
        for kind in range(9):
            copy(n, kind).wait_send()
    for c in whole:
        c.wait()


def exit_kernel(
    reps,
    ggp_ref, gup_ref, gw_ref, uw_ref, wd_ref, wg_ref, wu_ref,
    gn_ref, fd_ref, fg_ref, fu_ref,
    ind, ing, inu, tbuf, pin, sbuf, rsin,
    up_send, in_recv, fin_recv, down_send, p_send, p_recv, s_send, s_recv,
):
    f, t, r = lax.axis_index("fs"), lax.axis_index("tp"), lax.axis_index("rep")
    other = 1 - t
    middle = reps // 2
    sign = 1 - 2 * (r // middle)
    up, down = {"rep": r + sign}, {"rep": (r - sign + reps) % reps}
    right = r // middle
    depth = (1 - right) * (middle - 1 - r) + right * (r - middle)
    center, outer = depth == 0, depth == middle - 1
    inner, has_down = depth > 0, depth < middle - 1
    peers = [{"fs": flip(f, 1)}, {"fs": flip(f, 2)}, {"fs": flip(f, 3)}, {"tp": other}, up]
    barrier = pltpu.get_barrier_semaphore()
    for dev in peers:
        pl.semaphore_signal(barrier, inc=1, device_id=dev, device_id_type=MESH)

    @pl.when(has_down)
    def _():
        pl.semaphore_signal(barrier, inc=1, device_id=down, device_id_type=MESH)
        pl.semaphore_wait(barrier, 6)

    @pl.when(outer)
    def _():
        pl.semaphore_wait(barrier, 5)

    arrays = ((wd_ref, ind, fd_ref), (wg_ref, ing, fg_ref), (wu_ref, inu, fu_ref))
    rows = gn_ref.shape[0]
    width = gw_ref.shape[0]
    tile = min(512, width)

    def at(ref, s):
        step = ref.shape[0] // CHUNKS
        return ref.at[pl.ds(pl.multiple_of(s * step, step), step)]

    def up_copy(a, s, src, dst, recv):
        return remote(at(src, s), at(dst, s), up_send.at[a, s], recv.at[a, s], up)

    def down_copy(a, s):
        fin = arrays[a][2]
        return remote(at(fin, s), at(fin, s), down_send.at[a, s], fin_recv.at[a, s], down)

    @pl.when(outer)
    def _():
        def first(s, carry):
            for a, (own, inc, fin) in enumerate(arrays):
                up_copy(a, s, own, inc, in_recv).start()
            return carry

        lax.fori_loop(0, CHUNKS, first, 0)

    def pair_copy(j):
        return remote(tbuf.at[j], pin.at[j], p_send.at[j], p_recv.at[j], {"tp": other})

    def peer_copy(j):
        return remote(sbuf.at[j], rsin.at[j], s_send.at[j], s_recv.at[j], {"fs": flip(f, j)})

    def term(owner, c):
        here = pl.ds(pl.multiple_of(owner * rows, rows), rows)
        cols = pl.ds(pl.multiple_of(c * tile, tile), tile)
        out = lax.dot_general(ggp_ref[here, :], gw_ref[cols, :], NT, preferred_element_type=F32)
        out = out + lax.dot_general(gup_ref[here, :], uw_ref[cols, :], NT, preferred_element_type=F32)
        return out.astype(BF16), cols

    def body(s, carry):
        j = 3 - s % 4

        @pl.when(s < 4)
        def _():
            def one(c, carry):
                value, cols = term(flip(f, j) * 2 + other, c)
                tbuf[j, :, cols] = value
                return carry

            lax.fori_loop(0, width // tile, one, 0)
            pair_copy(j).start()

        @pl.when((s >= 4) & (s < 8))
        def _():
            pair_copy(j).wait_recv()

            def one(c, carry):
                value, cols = term(flip(f, j) * 2 + t, c)
                total = value.astype(F32) + pin[j, :, cols].astype(F32)
                gn_ref[:, cols] = total
                sbuf[j, :, cols] = total.astype(BF16)
                return carry

            lax.fori_loop(0, width // tile, one, 0)

            @pl.when(j > 0)
            def _():
                peer_copy(j).start()

        @pl.when((s < CHUNKS) & has_down)
        def _():
            for a, (own, inc, fin) in enumerate(arrays):
                up_copy(a, s, inc, inc, in_recv).wait_recv()
                here = at(inc, s)
                here[...] = (at(own, s)[...].astype(F32) + here[...].astype(F32)).astype(BF16)

                @pl.when(center)
                def _():
                    up_copy(a, s, inc, fin, fin_recv).start()

                @pl.when(inner)
                def _():
                    up_copy(a, s, inc, inc, in_recv).start()

        @pl.when(s >= 1)
        def _():
            for a, (own, inc, fin) in enumerate(arrays):
                before = s - 1
                down_copy(a, before).wait_recv()

                @pl.when(center)
                def _():
                    here = at(fin, before)
                    here[...] = (at(inc, before)[...].astype(F32) + here[...].astype(F32)).astype(BF16)

                @pl.when(has_down)
                def _():
                    down_copy(a, before).start()

        return carry

    lax.fori_loop(0, CHUNKS + 1, body, 0)
    for j in (3, 2, 1):
        peer_copy(j).wait_recv()
    gn_ref[...] = gn_ref[...] + rsin[3].astype(F32) + rsin[2].astype(F32) + rsin[1].astype(F32)
    for j in (3, 2, 1):
        peer_copy(j).wait_send()
    for j in range(4):
        pair_copy(j).wait_send()

    def last(s, carry):
        for a, (own, inc, fin) in enumerate(arrays):
            up_copy(a, s, own, inc, in_recv).wait_send()

            @pl.when(has_down)
            def _():
                down_copy(a, s).wait_send()

        return carry

    lax.fori_loop(0, CHUNKS, last, 0)


def shards(tokens_in, norm_gain, gate_weight, up_weight, down_weight, out_grad):
    rows, d = tokens_in.shape
    ff = gate_weight.shape[1]
    reps = lax.axis_size("rep")
    ranks = lax.axis_size("fs") * lax.axis_size("tp")
    factor = float(rows * reps * ranks) ** (-0.5)
    vmem, anywhere = pl.BlockSpec(memory_space=pltpu.VMEM), pl.BlockSpec(memory_space=pl.ANY)
    wide, narrow = (ranks, rows, d), (ranks, rows, ff)
    dma = pltpu.SemaphoreType.DMA
    flat = (ranks * rows,)
    gathered = pl.pallas_call(
        gather_kernel,
        out_shape=[jax.ShapeDtypeStruct(s, BF16) for s in (wide, wide, narrow, narrow, narrow)],
        in_specs=[vmem] * 6,
        out_specs=[anywhere] * 5,
        scratch_shapes=[
            pltpu.VMEM(wide, BF16), pltpu.VMEM(wide, BF16), pltpu.VMEM(wide, BF16),
            pltpu.VMEM(narrow, BF16), pltpu.VMEM(narrow, BF16), pltpu.VMEM(narrow, BF16),
            dma((2, 9)), dma((2, 9)), dma((5,)),
        ],
        compiler_params=pltpu.CompilerParams(
            collective_id=0, has_side_effects=True, vmem_limit_bytes=60 * 2**20
        ),
        name="gather_forward",
    )(tokens_in, out_grad, norm_gain.reshape(1, d), gate_weight, up_weight, down_weight)
    normed, whole_grad, hidden, ggp, gup = [a.reshape(flat + a.shape[2:]) for a in gathered]
    local_down = jnp.dot(hidden.T, whole_grad, preferred_element_type=F32).astype(BF16)
    local_gate = jnp.dot(normed.T, ggp, preferred_element_type=F32).astype(BF16)
    local_up = jnp.dot(normed.T, gup, preferred_element_type=F32).astype(BF16)
    tall, long = (d, ff), (ff, d)
    block4 = (4, rows, d)
    grad_normed, sum_down, sum_gate, sum_up = pl.pallas_call(
        lambda *refs: exit_kernel(reps, *refs),
        out_shape=[
            jax.ShapeDtypeStruct((rows, d), F32),
            jax.ShapeDtypeStruct(long, BF16),
            jax.ShapeDtypeStruct(tall, BF16),
            jax.ShapeDtypeStruct(tall, BF16),
        ],
        in_specs=[vmem] * 7,
        out_specs=[vmem] * 4,
        scratch_shapes=[
            pltpu.VMEM(long, BF16), pltpu.VMEM(tall, BF16), pltpu.VMEM(tall, BF16),
            pltpu.VMEM(block4, BF16), pltpu.VMEM(block4, BF16), pltpu.VMEM(block4, BF16), pltpu.VMEM(block4, BF16),
            dma((3, CHUNKS)), dma((3, CHUNKS)), dma((3, CHUNKS)), dma((3, CHUNKS)),
            dma((4,)), dma((4,)), dma((4,)), dma((4,)),
        ],
        compiler_params=pltpu.CompilerParams(
            collective_id=1, has_side_effects=True, vmem_limit_bytes=60 * 2**20
        ),
        name="reduce_exit",
    )(ggp, gup, gate_weight, up_weight, local_down, local_gate, local_up)
    grad_gate = sum_gate.astype(F32) * factor
    grad_up = sum_up.astype(F32) * factor
    grad_down = sum_down.astype(F32) * (0.5 * factor)
    floats = tokens_in.astype(F32)
    inverse = lax.rsqrt(jnp.mean(floats * floats, axis=-1, keepdims=True) + norm_eps)
    unit = floats * inverse
    grad_gain = lax.psum(jnp.sum(grad_normed * unit, axis=0), ("rep", "fs", "tp"))
    scaled = grad_normed * norm_gain
    grad_in = (
        out_grad.astype(F32)
        + inverse * scaled
        - unit * inverse * jnp.mean(scaled * unit, axis=-1, keepdims=True)
    )
    return (grad_in.astype(BF16), grad_gain, grad_gate, grad_up, grad_down)


def solution(mesh):
    spread = ("fs", "tp")
    in_specs = (
        P(("rep", "fs", "tp"), None), P(), P(None, spread), P(None, spread), P(spread, None),
        P(("rep", "fs", "tp"), None),
    )
    out_specs = (
        P(("rep", "fs", "tp"), None), P(), P(None, spread), P(None, spread), P(spread, None),
    )
    return jax.shard_map(shards, mesh=mesh, in_specs=in_specs, out_specs=out_specs, check_vma=False)
```

```python
import jax
import jax.numpy as jnp
from jax import lax
from jax.experimental import pallas as pl
from jax.experimental.pallas import tpu as pltpu
from jax.sharding import PartitionSpec as P

norm_eps = 1e-06
MESH = pl.DeviceIdType.MESH
F32, BF16 = jnp.float32, jnp.bfloat16
CHUNKS = 8
NT = (((1,), (1,)), ((), ()))


def flip(f, j):
    return (f % 2 + j % 2) % 2 + 2 * ((f // 2 + j // 2) % 2)


def remote(src, dst, send, recv, dev):
    return pltpu.make_async_remote_copy(
        src_ref=src, dst_ref=dst, send_sem=send, recv_sem=recv, device_id=dev, device_id_type=MESH
    )


def gather_kernel(
    x_ref, g_ref, gain_ref, gw_ref, uw_ref, dw_ref,
    normed_out, grad_out, hid_out, ggp_out, gup_out,
    xall, gall, normed, hid, ggp, gup, ssem, rsem, osem,
):
    f, t = lax.axis_index("fs"), lax.axis_index("tp")
    other = 1 - t
    rows = x_ref.shape[0]
    half = rows // 2
    to_a, to_b, to_p = {"fs": flip(f, 1)}, {"fs": flip(f, 2)}, {"tp": other}
    barrier = pltpu.get_barrier_semaphore()
    for dev in (to_a, to_b, to_p):
        pl.semaphore_signal(barrier, inc=1, device_id=dev, device_id_type=MESH)
    pl.semaphore_wait(barrier, 3)

    def pos(j, core):
        return flip(f, j) * 2 + core

    bufs = ((x_ref, xall), (g_ref, gall))
    low, high = pl.ds(0, half), pl.ds(half, half)

    def copy(n, kind, incoming=False):
        own, held = bufs[n]
        sems = (ssem.at[n, kind], rsem.at[n, kind])
        mine = pos(0, t)
        if kind == 0:
            return remote(own, held.at[pos(1, t) if incoming else mine], *sems, to_a)
        if kind == 1:
            return remote(own, held.at[pos(2, t) if incoming else mine], *sems, to_b)
        if kind == 2:
            return remote(own, held.at[pos(0, other) if incoming else mine], *sems, to_p)
        if kind == 3:
            slot = held.at[pos(3, t) if incoming else pos(1, t), high]
            return remote(slot, slot, *sems, to_b)
        if kind == 4:
            slot = held.at[pos(3, t) if incoming else pos(2, t), low]
            return remote(slot, slot, *sems, to_a)
        j = {5: 1, 6: 2, 7: 3, 8: 3}[kind]
        slot = held.at[pos(j, other if incoming else t)]
        if kind == 7:
            slot = slot.at[low]
        if kind == 8:
            slot = slot.at[high]
        return remote(slot, slot, *sems, to_p)

    for n in range(2):
        for kind in (0, 1, 2):
            copy(n, kind).start()
    xall[pos(0, t)] = x_ref[...]
    gall[pos(0, t)] = g_ref[...]

    def body(i, carry):
        @pl.when(i == 1)
        def _():
            for n in range(2):
                copy(n, 2, True).wait_recv()

        @pl.when(i == 2)
        def _():
            for n in range(2):
                copy(n, 0, True).wait_recv()
                copy(n, 3).start()
                copy(n, 5).start()
                copy(n, 1, True).wait_recv()
                copy(n, 4).start()
                copy(n, 6).start()

        @pl.when(i == 3)
        def _():
            for n in range(2):
                copy(n, 5, True).wait_recv()

        @pl.when(i == 5)
        def _():
            for n in range(2):
                copy(n, 6, True).wait_recv()

        @pl.when(i == 6)
        def _():
            for n in range(2):
                copy(n, 4, True).wait_recv()
                copy(n, 7).start()
                copy(n, 3, True).wait_recv()
                copy(n, 8).start()

        @pl.when(i == 7)
        def _():
            for n in range(2):
                copy(n, 7, True).wait_recv()
                copy(n, 8, True).wait_recv()

        p = flip(f, i // 2) * 2 + (t + i) % 2
        floats = xall[p].astype(F32)
        inverse = lax.rsqrt(jnp.mean(floats * floats, axis=-1, keepdims=True) + norm_eps)
        normed[p] = (floats * inverse * gain_ref[...]).astype(BF16)
        gate_pre = jnp.dot(normed[p], gw_ref[...], preferred_element_type=F32)
        up_pre = jnp.dot(normed[p], uw_ref[...], preferred_element_type=F32)
        grad_hidden = 0.5 * lax.dot_general(gall[p], dw_ref[...], NT, preferred_element_type=F32)
        sigma = jax.nn.sigmoid(gate_pre)
        active = gate_pre * sigma
        hid[p] = (active * up_pre).astype(BF16)
        ggp[p] = (grad_hidden * up_pre * sigma * (1.0 + gate_pre * (1.0 - sigma))).astype(BF16)
        gup[p] = (grad_hidden * active).astype(BF16)
        return carry

    lax.fori_loop(0, 8, body, 0)
    whole = [
        pltpu.make_async_copy(src, dst, osem.at[i])
        for i, (src, dst) in enumerate(
            ((normed, normed_out), (gall, grad_out), (hid, hid_out), (ggp, ggp_out), (gup, gup_out))
        )
    ]
    for c in whole:
        c.start()
    for n in range(2):
        for kind in range(9):
            copy(n, kind).wait_send()
    for c in whole:
        c.wait()


def exit_kernel(
    reps,
    x_ref, ggp_ref, gup_ref, gw_ref, uw_ref, wd_ref, wg_ref, wu_ref,
    gn_ref, gain_ref, fd_ref, fg_ref, fu_ref,
    ind, ing, inu, tbuf, pin, sbuf, rsin, gbuf, rbuf,
    up_send, in_recv, fin_recv, down_send, p_send, p_recv, s_send, s_recv,
    g_send, g_recv, r_send, r_recv,
):
    f, t, r = lax.axis_index("fs"), lax.axis_index("tp"), lax.axis_index("rep")
    other = 1 - t
    middle = reps // 2
    sign = 1 - 2 * (r // middle)
    up, down = {"rep": r + sign}, {"rep": (r - sign + reps) % reps}
    right = r // middle
    depth = (1 - right) * (middle - 1 - r) + right * (r - middle)
    center, outer = depth == 0, depth == middle - 1
    inner, has_down = depth > 0, depth < middle - 1
    group = []
    for j in range(4):
        for k in range(2):
            if j or k:
                core = (t + k) % 2
                group.append((flip(f, j) * 2 + core, {"fs": flip(f, j), "tp": core}))
    far = [((r + k) % reps, (r - k + reps) % reps) for k in range(1, reps)]
    barrier = pltpu.get_barrier_semaphore()
    for dev in [dev for _, dev in group] + [{"rep": to} for to, _ in far]:
        pl.semaphore_signal(barrier, inc=1, device_id=dev, device_id_type=MESH)
    pl.semaphore_wait(barrier, len(group) + len(far))

    arrays = ((wd_ref, ind, fd_ref), (wg_ref, ing, fg_ref), (wu_ref, inu, fu_ref))
    rows = gn_ref.shape[0]
    width = gw_ref.shape[0]
    tile = min(512, width)

    def at(ref, s):
        step = ref.shape[0] // CHUNKS
        return ref.at[pl.ds(pl.multiple_of(s * step, step), step)]

    def up_copy(a, s, src, dst, recv):
        return remote(at(src, s), at(dst, s), up_send.at[a, s], recv.at[a, s], up)

    def down_copy(a, s):
        fin = arrays[a][2]
        return remote(at(fin, s), at(fin, s), down_send.at[a, s], fin_recv.at[a, s], down)

    @pl.when(outer)
    def _():
        def first(s, carry):
            for a, (own, inc, fin) in enumerate(arrays):
                up_copy(a, s, own, inc, in_recv).start()
            return carry

        lax.fori_loop(0, CHUNKS, first, 0)

    def pair_copy(j):
        return remote(tbuf.at[j], pin.at[j], p_send.at[j], p_recv.at[j], {"tp": other})

    def peer_copy(j):
        return remote(sbuf.at[j], rsin.at[j], s_send.at[j], s_recv.at[j], {"fs": flip(f, j)})

    def term(owner, c):
        here = pl.ds(pl.multiple_of(owner * rows, rows), rows)
        cols = pl.ds(pl.multiple_of(c * tile, tile), tile)
        out = lax.dot_general(ggp_ref[here, :], gw_ref[cols, :], NT, preferred_element_type=F32)
        out = out + lax.dot_general(gup_ref[here, :], uw_ref[cols, :], NT, preferred_element_type=F32)
        return out.astype(BF16), cols

    mine = f * 2 + t

    def group_copy(n, incoming=False):
        where, dev = group[n]
        slot = gbuf.at[where if incoming else mine]
        return remote(gbuf.at[mine], slot, g_send.at[n], g_recv.at[n], dev)

    def far_copy(n, incoming=False):
        to, source = far[n]
        slot = rbuf.at[source if incoming else r]
        return remote(rbuf.at[r], slot, r_send.at[n], r_recv.at[n], {"rep": to})

    def for_partner(i, carry):
        j = 3 - i

        def one(c, carry):
            value, cols = term(flip(f, j) * 2 + other, c)
            tbuf[j, :, cols] = value
            return carry

        lax.fori_loop(0, width // tile, one, 0)
        pair_copy(j).start()
        return carry

    lax.fori_loop(0, 4, for_partner, 0)

    def inward(a, s):
        own, inc, fin = arrays[a]

        @pl.when(has_down)
        def _():
            up_copy(a, s, inc, inc, in_recv).wait_recv()
            here = at(inc, s)
            here[...] = (at(own, s)[...].astype(F32) + here[...].astype(F32)).astype(BF16)

            @pl.when(center)
            def _():
                up_copy(a, s, inc, fin, fin_recv).start()

            @pl.when(inner)
            def _():
                up_copy(a, s, inc, inc, in_recv).start()

    def outward(a, s):
        own, inc, fin = arrays[a]
        down_copy(a, s).wait_recv()

        @pl.when(center)
        def _():
            here = at(fin, s)
            here[...] = (at(inc, s)[...].astype(F32) + here[...].astype(F32)).astype(BF16)

        @pl.when(has_down)
        def _():
            down_copy(a, s).start()

    def body(s, carry):
        j = 3 - s % 4

        @pl.when(s < 4)
        def _():
            pair_copy(j).wait_recv()

            def one(c, carry):
                value, cols = term(flip(f, j) * 2 + t, c)
                total = value.astype(F32) + pin[j, :, cols].astype(F32)
                gn_ref[:, cols] = total
                sbuf[j, :, cols] = total.astype(BF16)
                return carry

            lax.fori_loop(0, width // tile, one, 0)

            @pl.when(j > 0)
            def _():
                peer_copy(j).start()

        for a in range(3):

            @pl.when(s < CHUNKS)
            def _():
                inward(a, s)

            if a < 2:

                @pl.when(s >= 1)
                def _():
                    outward(a + 1, s - 1)

            else:

                @pl.when(s < CHUNKS)
                def _():
                    outward(0, s)

        @pl.when(s == CHUNKS - 1)
        def _():
            for k in (3, 2, 1):
                peer_copy(k).wait_recv()

            def one(c, carry):
                cols = pl.ds(pl.multiple_of(c * tile, tile), tile)
                total = gn_ref[:, cols]
                for k in (3, 2, 1):
                    total = total + rsin[k, :, cols].astype(F32)
                gn_ref[:, cols] = total
                return carry

            lax.fori_loop(0, width // tile, one, 0)
            floats = x_ref[...].astype(F32)
            inverse = lax.rsqrt(jnp.mean(floats * floats, axis=-1, keepdims=True) + norm_eps)
            gbuf[mine] = jnp.sum(gn_ref[...] * (floats * inverse), axis=0, keepdims=True)
            for n in range(len(group)):
                group_copy(n).start()

        return carry

    lax.fori_loop(0, CHUNKS + 1, body, 0)
    for n in range(len(group)):
        group_copy(n, True).wait_recv()
    rbuf[r] = jnp.sum(gbuf[...], axis=0)
    for n in range(len(far)):
        far_copy(n).start()
    for n in range(len(far)):
        far_copy(n, True).wait_recv()
    gain_ref[...] = jnp.sum(rbuf[...], axis=0)
    for n in range(len(group)):
        group_copy(n).wait_send()
    for n in range(len(far)):
        far_copy(n).wait_send()
    for j in (3, 2, 1):
        peer_copy(j).wait_send()
    for j in range(4):
        pair_copy(j).wait_send()

    def last(s, carry):
        for a, (own, inc, fin) in enumerate(arrays):
            up_copy(a, s, own, inc, in_recv).wait_send()

            @pl.when(has_down)
            def _():
                down_copy(a, s).wait_send()

        return carry

    lax.fori_loop(0, CHUNKS, last, 0)


def shards(tokens_in, norm_gain, gate_weight, up_weight, down_weight, out_grad):
    rows, d = tokens_in.shape
    ff = gate_weight.shape[1]
    reps = lax.axis_size("rep")
    ranks = lax.axis_size("fs") * lax.axis_size("tp")
    factor = float(rows * reps * ranks) ** (-0.5)
    vmem, anywhere = pl.BlockSpec(memory_space=pltpu.VMEM), pl.BlockSpec(memory_space=pl.ANY)
    wide, narrow = (ranks, rows, d), (ranks, rows, ff)
    dma = pltpu.SemaphoreType.DMA
    flat = (ranks * rows,)
    gathered = pl.pallas_call(
        gather_kernel,
        out_shape=[jax.ShapeDtypeStruct(s, BF16) for s in (wide, wide, narrow, narrow, narrow)],
        in_specs=[vmem] * 6,
        out_specs=[anywhere] * 5,
        scratch_shapes=[
            pltpu.VMEM(wide, BF16), pltpu.VMEM(wide, BF16), pltpu.VMEM(wide, BF16),
            pltpu.VMEM(narrow, BF16), pltpu.VMEM(narrow, BF16), pltpu.VMEM(narrow, BF16),
            dma((2, 9)), dma((2, 9)), dma((5,)),
        ],
        compiler_params=pltpu.CompilerParams(
            collective_id=0, has_side_effects=True, vmem_limit_bytes=60 * 2**20
        ),
        name="gather_forward",
    )(tokens_in, out_grad, norm_gain.reshape(1, d), gate_weight, up_weight, down_weight)
    normed, whole_grad, hidden, ggp, gup = [a.reshape(flat + a.shape[2:]) for a in gathered]
    local_down = jnp.dot(hidden.T, whole_grad, preferred_element_type=F32).astype(BF16)
    local_gate = jnp.dot(normed.T, ggp, preferred_element_type=F32).astype(BF16)
    local_up = jnp.dot(normed.T, gup, preferred_element_type=F32).astype(BF16)
    tall, long = (d, ff), (ff, d)
    block4 = (4, rows, d)
    grad_normed, grad_gain, sum_down, sum_gate, sum_up = pl.pallas_call(
        lambda *refs: exit_kernel(reps, *refs),
        out_shape=[
            jax.ShapeDtypeStruct((rows, d), F32),
            jax.ShapeDtypeStruct((1, d), F32),
            jax.ShapeDtypeStruct(long, BF16),
            jax.ShapeDtypeStruct(tall, BF16),
            jax.ShapeDtypeStruct(tall, BF16),
        ],
        in_specs=[vmem] * 8,
        out_specs=[vmem] * 5,
        scratch_shapes=[
            pltpu.VMEM(long, BF16), pltpu.VMEM(tall, BF16), pltpu.VMEM(tall, BF16),
            pltpu.VMEM(block4, BF16), pltpu.VMEM(block4, BF16), pltpu.VMEM(block4, BF16), pltpu.VMEM(block4, BF16),
            pltpu.VMEM((ranks, 1, d), F32), pltpu.VMEM((reps, 1, d), F32),
            dma((3, CHUNKS)), dma((3, CHUNKS)), dma((3, CHUNKS)), dma((3, CHUNKS)),
            dma((4,)), dma((4,)), dma((4,)), dma((4,)),
            dma((ranks,)), dma((ranks,)), dma((reps,)), dma((reps,)),
        ],
        compiler_params=pltpu.CompilerParams(
            collective_id=1, has_side_effects=True, vmem_limit_bytes=60 * 2**20
        ),
        name="reduce_exit",
    )(tokens_in, ggp, gup, gate_weight, up_weight, local_down, local_gate, local_up)
    grad_gate = sum_gate.astype(F32) * factor
    grad_up = sum_up.astype(F32) * factor
    grad_down = sum_down.astype(F32) * (0.5 * factor)
    floats = tokens_in.astype(F32)
    inverse = lax.rsqrt(jnp.mean(floats * floats, axis=-1, keepdims=True) + norm_eps)
    unit = floats * inverse
    scaled = grad_normed * norm_gain
    grad_in = (
        out_grad.astype(F32)
        + inverse * scaled
        - unit * inverse * jnp.mean(scaled * unit, axis=-1, keepdims=True)
    )
    return (grad_in.astype(BF16), grad_gain.reshape(d), grad_gate, grad_up, grad_down)


def solution(mesh):
    spread = ("fs", "tp")
    in_specs = (
        P(("rep", "fs", "tp"), None), P(), P(None, spread), P(None, spread), P(spread, None),
        P(("rep", "fs", "tp"), None),
    )
    out_specs = (
        P(("rep", "fs", "tp"), None), P(), P(None, spread), P(None, spread), P(spread, None),
    )
    return jax.shard_map(shards, mesh=mesh, in_specs=in_specs, out_specs=out_specs, check_vma=False)
```
